32 devices in a mesh: ep: 8 (over z, x), tp: 4 (over y, core).
Axes of the slice: x: 2, y: 2, z: 4, core: 2. Of those that a mesh axis runs over, the one named last changes fastest.
Arguments:
- head_inputs_unfiltered: bfloat16 [1024, 4096], P('ep', 'tp'), may hold values from -6 to 6
- group_write_vectors: bfloat16 [1024, 512], P('ep', 'tp'), may hold values from -6 to 6
- group_read_vectors: bfloat16 [1024, 512], P('ep', 'tp'), may hold values from -6 to 6
- output_gate_inputs: bfloat16 [1024, 4096], P('ep', 'tp'), may hold values from -6 to 6
- step_preactivation: float32 [64, 1024], P('tp', 'ep'), may hold values from -3.2 to 3.6
- extra_decay_logs: float32 [64, 1024], P('tp', 'ep'), may hold values from -0.7 to 0
- head_decay_logs: float32 [64], P('tp'), may hold values from -16 to -2.7
- head_filter_taps: bfloat16 [4, 4096], P(None, 'tp'), may hold values from -3 to 3
- write_filter_taps: bfloat16 [4, 512], P(None, 'tp'), may hold values from -3 to 3
- read_filter_taps: bfloat16 [4, 512], P(None, 'tp'), may hold values from -3 to 3
- grouped_norm_gain: float32 [4096], P('tp'), may hold values from 0.1 to 1.9
- mixer_output_weight: bfloat16 [4096, 2048], P('tp'), may hold values from -0.09375 to 0.09375
- expert_input_rows: bfloat16 [4096, 2048], P(('ep', 'tp')), may hold values from -6 to 6
- expert_norm_gain: float32 [2048], replicated, may hold values from 0.1 to 1.9
- routes: int32 [4096, 2], P(('ep', 'tp')), may hold values from 0 to 7, all different within a row; in each aligned block of 128 rows (0 to 127, 128 to 255, ...) at most 48 rows name the same one
- router_chosen_scores: bfloat16 [4096, 2], P(('ep', 'tp')), may hold values from 0.049804688 to 1
- routed_gate_weight: bfloat16 [8, 2048, 1024], P('ep', None, 'tp'), may hold values from -0.125 to 0.125
- routed_up_weight: bfloat16 [8, 2048, 1024], P('ep', None, 'tp'), may hold values from -0.125 to 0.125
- routed_down_weight: bfloat16 [8, 1024, 2048], P('ep', 'tp'), may hold values from -0.1875 to 0.1875
- shared_gate_weight: bfloat16 [2048, 512], P(None, 'tp'), may hold values from -0.125 to 0.125
- shared_up_weight: bfloat16 [2048, 512], P(None, 'tp'), may hold values from -0.125 to 0.125
- shared_down_weight: bfloat16 [512, 2048], P('tp'), may hold values from -0.25 to 0.25
Outputs:
- mixer_result: bfloat16 [1024, 2048], P(('ep', 'tp'))
- moe_result: bfloat16 [4096, 2048], P(('ep', 'tp'))
The draws below stay inside these ranges and needn't reach their ends.
Inputs may be any that keep to these rules, and one draw needn't show every extreme that they name: `routes`: within the 128 rows of one device no expert is named more than 48 times; a row names 2 different experts.
All inputs are finite; a program needn't handle non-finite values.
Results may differ from the reference program's by a relative error of at most 0.0095.
Values may be sent and summed in bfloat16 or wider, within the bound.
A program may use at most 128 MiB of HBM per device.

```python
import math
import jax
import jax.numpy as jnp
import numpy as np
from jax import lax

D = 2048
HEADS = 64
HEAD_DIM = 64
GROUPS = 4
STATE = 128
CONV = 4
BLOCK = 64
INNER = 4096
MIX_ROWS = 128
MIX_TOKENS = 1024
EXPERT_FF = 1024
SHARED_FF = 512
EXPERTS = 8
TOP_K = 2
MOE_ROWS = 128
MOE_TOKENS = 4096
CAPACITY = 48
N_TP = 4


def draw_step_preactivation(key, part):
    key_noise, key_shift = jax.random.split(key)
    block_total = MIX_TOKENS // MIX_ROWS
    noise = jnp.clip(0.7 * jax.random.normal(key_noise, (HEADS, MIX_TOKENS), jnp.float32), -1.6, 1.6)
    shifts = jax.random.uniform(key_shift, (block_total,), jnp.float32, -1.0, 1.5)
    return noise + jnp.repeat(shifts, MIX_ROWS)[None, :]


def draw_extra_decay_logs(key, part):
    key_place, key_depth = jax.random.split(key)
    stride = MIX_TOKENS // 3
    places = jnp.arange(3, dtype=jnp.int32) * stride + jax.random.randint(key_place, (3,), 0, stride)
    kept = jax.random.uniform(key_depth, (3, HEADS), jnp.float32, 0.5, 0.8)
    positions = jnp.arange(MIX_TOKENS, dtype=jnp.int32)
    hits = (positions[None, :] == places[:, None]).astype(jnp.float32)
    return jnp.einsum('bh,bt->ht', jnp.log(kept), hits)


def draw_head_decay_logs(key, part):
    key_kind, key_fast, key_slow = jax.random.split(key, 3)
    fast_share = 0.5
    is_fast = jax.random.uniform(key_kind, (HEADS,), jnp.float32) < fast_share
    fast_log = jax.random.uniform(key_fast, (HEADS,), jnp.float32, math.log(1.0 / 40.0), math.log(1.0 / 15.0))
    slow_log = jax.random.uniform(key_slow, (HEADS,), jnp.float32, math.log(0.02), math.log(0.25)) - math.log(float(MIX_TOKENS))
    return jnp.where(is_fast, fast_log, slow_log)


def shard_levels(key, shape, cuts, smallest, high):
    loudness, own = 1.0, jax.random.fold_in(key, 6)
    for position, blocks in cuts:
        draws = jnp.exp(jax.random.uniform(jax.random.fold_in(own, position), (blocks,), jnp.float32, smallest / len(cuts), high / len(cuts)))
        loudness = loudness * jnp.repeat(draws, shape[position] // blocks).reshape([-1 if axis == position else 1 for axis in range(len(shape))])
    return loudness


def deal_out(key, own, number, rows, amount, top, limit, skew):
    sequence = jax.random.permutation(key, amount)
    packed, ordinary = load_shares(amount, rows * top, limit, skew, True), load_shares(amount, rows * top, limit, skew, False)
    places = jnp.arange(amount)

    def named(tallies, rotation):
        used = int((tallies > 0).sum())
        fixed = max(1, used // 4)
        passed = fixed + (places - fixed + rotation * (used - fixed)) % max(1, amount - fixed)
        return jnp.zeros((amount,), jnp.int32).at[sequence[jnp.where(places < fixed, places, passed)]].set(jnp.asarray(tallies, jnp.int32))

    tallies = jnp.where(number % 4 == 0, named(packed, number // 4), named(ordinary, number - number // 4 - 1))
    mixed = jax.random.permutation(jax.random.fold_in(own, 3), amount)
    giver, taker = mixed[0:amount // 2 * 2:2], mixed[1:amount // 2 * 2:2]
    margin = jnp.minimum(tallies[giver] - 1, limit - tallies[taker]) // 2
    margin = jnp.where((giver == sequence[0]) | (taker == sequence[0]) | (tallies[taker] == 0), 0, jnp.maximum(margin, 0))
    passed = jax.random.randint(jax.random.fold_in(own, 4), (amount // 2,), 0, 1 << 20) % (margin + 1)
    tallies = tallies.at[giver].add(-passed).at[taker].add(passed)
    items = jnp.searchsorted(jnp.cumsum(tallies), jnp.arange(rows * top), side="right").astype(jnp.int32)
    grid = items.reshape(top, rows).T
    grid = grid[jax.random.permutation(jax.random.fold_in(own, 1), rows)]
    rotation = jax.random.randint(jax.random.fold_in(own, 2), (rows, 1), 0, top)
    return jnp.take_along_axis(grid, (jnp.arange(top)[None, :] + rotation) % top, axis=1)


def load_shares(number_of, total, most, lean, full):
    weights = [(1 << 20) // math.isqrt(grade ** lean) + 1 for grade in range(1, number_of + 1)]
    largest = most if full else min(most, max(-(-total // number_of), total * weights[0] // sum(weights)))
    least = 1 if total - largest >= number_of - 1 else 0
    counts, surplus = [largest] + [least] * (number_of - 1), total - largest - least * (number_of - 1)
    while surplus > 0:
        candidates = [i for i in range(1, number_of) if counts[i] < largest] or [i for i in range(1, number_of) if counts[i] < most]
        whole, remaining = sum([weights[i] for i in candidates]), surplus
        for i in candidates:
            more = min(most - counts[i], max(1, remaining * weights[i] // whole), surplus)
            counts[i] = counts[i] + more
            surplus = surplus - more
    return np.array(counts)


def scatter_about(key, dims, deviation, bound, pieces=(), kind=jnp.bfloat16):
    level = shard_levels(key, dims, pieces, -0.22, 0.18) if pieces else 1.0
    result = jax.random.normal(key, dims, jnp.float32) * deviation * level
    return jnp.minimum(jnp.maximum(result, -bound), bound).astype(kind)


def setup_inputs(seed: int = 0) -> dict:
    streams_of = jax.random.split(jax.random.key(seed), 23)
    head_inputs_unfiltered = scatter_about(streams_of[0], (MIX_TOKENS, INNER), 1.0, 6.0, ((0, 8), (1, 4)))
    group_write_vectors = scatter_about(streams_of[1], (MIX_TOKENS, GROUPS * STATE), 1.0, 6.0, ((0, 8), (1, 4)))
    group_read_vectors = scatter_about(streams_of[2], (MIX_TOKENS, GROUPS * STATE), 1.0, 6.0, ((0, 8), (1, 4)))
    output_gate_inputs = scatter_about(streams_of[3], (MIX_TOKENS, INNER), 1.0, 6.0, ((0, 8), (1, 4)))
    step_preactivation = draw_step_preactivation(jax.random.fold_in(streams_of[22], 71), 0)
    extra_decay_logs = draw_extra_decay_logs(jax.random.fold_in(streams_of[22], 71), 0)
    head_decay_logs = draw_head_decay_logs(jax.random.fold_in(streams_of[22], 71), 0)
    head_filter_taps = scatter_about(streams_of[7], (CONV, INNER), 0.5, 3.0, ((1, 4),))
    write_filter_taps = scatter_about(streams_of[8], (CONV, GROUPS * STATE), 0.5, 3.0, ((1, 4),))
    read_filter_taps = scatter_about(streams_of[9], (CONV, GROUPS * STATE), 0.5, 3.0, ((1, 4),))
    grouped_norm_gain = jnp.clip(1.0 + 0.18 * jax.random.normal(streams_of[10], (INNER,), jnp.float32), 0.1, 1.9)
    mixer_output_weight = scatter_about(streams_of[11], (INNER, D), INNER ** -0.5, 0.09375, ((0, 4),))
    expert_input_rows = scatter_about(streams_of[12], (MOE_TOKENS, D), 1.0, 6.0, ((0, 32),))
    expert_norm_gain = jnp.clip(1.0 + 0.18 * jax.random.normal(streams_of[13], (D,), jnp.float32), 0.1, 1.9)
    routes_keys = jax.random.split(jax.random.fold_in(streams_of[14], 1), MOE_TOKENS // MOE_ROWS)
    routes_turns = jax.random.permutation(jax.random.fold_in(streams_of[14], 3), MOE_TOKENS // MOE_ROWS)
    routes = jax.vmap(lambda own, number: deal_out(jax.random.fold_in(streams_of[14], 2), own, number, MOE_ROWS, EXPERTS, TOP_K, CAPACITY, 2))(routes_keys, routes_turns).reshape((MOE_TOKENS, TOP_K))
    router_chosen_scores = jnp.clip(jnp.exp(math.log(1.0) - 2.9996462 * jax.random.uniform(streams_of[15], (MOE_TOKENS, TOP_K), jnp.float32) ** shard_levels(streams_of[15], (MOE_TOKENS, TOP_K), ((0, 32),), -0.2, 0.2)), 0.049804688, 1.0).astype(jnp.bfloat16)
    routed_gate_weight = scatter_about(streams_of[16], (EXPERTS, D, EXPERT_FF), D ** -0.5, 0.125, ((0, 8), (2, 4)))
    routed_up_weight = scatter_about(streams_of[17], (EXPERTS, D, EXPERT_FF), D ** -0.5, 0.125, ((0, 8), (2, 4)))
    routed_down_weight = scatter_about(streams_of[18], (EXPERTS, EXPERT_FF, D), EXPERT_FF ** -0.5, 0.1875, ((0, 8), (1, 4)))
    shared_gate_weight = scatter_about(streams_of[19], (D, SHARED_FF), D ** -0.5, 0.125, ((1, 4),))
    shared_up_weight = scatter_about(streams_of[20], (D, SHARED_FF), D ** -0.5, 0.125, ((1, 4),))
    shared_down_weight = scatter_about(streams_of[21], (SHARED_FF, D), SHARED_FF ** -0.5, 0.25, ((0, 4),))
    return dict(head_inputs_unfiltered=head_inputs_unfiltered, group_write_vectors=group_write_vectors, group_read_vectors=group_read_vectors, output_gate_inputs=output_gate_inputs, step_preactivation=step_preactivation, extra_decay_logs=extra_decay_logs, head_decay_logs=head_decay_logs, head_filter_taps=head_filter_taps, write_filter_taps=write_filter_taps, read_filter_taps=read_filter_taps, grouped_norm_gain=grouped_norm_gain, mixer_output_weight=mixer_output_weight, expert_input_rows=expert_input_rows, expert_norm_gain=expert_norm_gain, routes=routes, router_chosen_scores=router_chosen_scores, routed_gate_weight=routed_gate_weight, routed_up_weight=routed_up_weight, routed_down_weight=routed_down_weight, shared_gate_weight=shared_gate_weight, shared_up_weight=shared_up_weight, shared_down_weight=shared_down_weight)


eps_norm = 1e-06
route_scale = 2.5
highest = lax.Precision.HIGHEST

def causal_conv(values, weights):
    taps = weights.shape[0]
    length = values.shape[0]
    padded = jnp.concatenate([jnp.zeros((taps - 1, values.shape[1]), jnp.float32), values.astype(jnp.float32)], axis=0)
    running_sum = jnp.zeros((length, values.shape[1]), jnp.float32)
    for offset in range(taps):
        running_sum = running_sum + weights[offset].astype(jnp.float32) * padded[offset:offset + length]
    return jax.nn.silu(running_sum)

def state_space(head_values, write_values, read_values, step_length_value, decay_rate_logs):
    length = head_values.shape[0]
    block_count = length // BLOCK
    per_group = HEADS // GROUPS
    head_blocks = head_values.reshape(block_count, BLOCK, GROUPS, per_group, HEAD_DIM)
    write_blocks = write_values.reshape(block_count, BLOCK, GROUPS, STATE)
    read_blocks = read_values.reshape(block_count, BLOCK, GROUPS, STATE)
    step_blocks = step_length_value.T.reshape(block_count, BLOCK, GROUPS, per_group)
    rate_blocks = decay_rate_logs.T.reshape(block_count, BLOCK, GROUPS, per_group)
    lower_mask = jnp.tril(jnp.ones((BLOCK, BLOCK), bool))

    def advance(carried, block_data):
        head_blk, write_blk, read_blk, step_blk, rate_blk = block_data
        cumulative = jnp.cumsum(rate_blk, axis=0)
        weighted = head_blk * step_blk[..., None]
        gap_logs = cumulative[:, None] - cumulative[None, :]
        within = jnp.exp(jnp.where(lower_mask[:, :, None, None], gap_logs, -jnp.inf))
        affinity = jnp.einsum('lgn,sgn->lsg', read_blk, write_blk, precision=highest)
        local_part = jnp.einsum('lsge,sgep->lgep', affinity[..., None] * within, weighted, precision=highest)
        carried_part = jnp.einsum('lgn,gepn->lgep', read_blk, carried, precision=highest) * jnp.exp(cumulative)[..., None]
        to_end = jnp.exp(cumulative[-1:] - cumulative)
        new_state = carried * jnp.exp(cumulative[-1])[..., None, None] + jnp.einsum('sgn,sgep->gepn', write_blk, weighted * to_end[..., None], precision=highest)
        return (new_state, local_part + carried_part)
    initial = jnp.zeros((GROUPS, per_group, HEAD_DIM, STATE), jnp.float32)
    _, outputs = lax.scan(advance, initial, (head_blocks, write_blocks, read_blocks, step_blocks, rate_blocks))
    return outputs.reshape(length, HEADS * HEAD_DIM)

def reference(head_inputs_unfiltered, group_write_vectors, group_read_vectors, output_gate_inputs, step_preactivation, extra_decay_logs, head_decay_logs, head_filter_taps, write_filter_taps, read_filter_taps, grouped_norm_gain, mixer_output_weight, expert_input_rows, expert_norm_gain, routes, router_chosen_scores, routed_gate_weight, routed_up_weight, routed_down_weight, shared_gate_weight, shared_up_weight, shared_down_weight):
    length = head_inputs_unfiltered.shape[0]
    head_values = causal_conv(head_inputs_unfiltered, head_filter_taps)
    write_values = causal_conv(group_write_vectors, write_filter_taps)
    read_values = causal_conv(group_read_vectors, read_filter_taps)
    step_length_value = jax.nn.softplus(step_preactivation)
    decay_rate_logs = -jnp.exp(head_decay_logs)[:, None] * step_length_value + extra_decay_logs
    scan_out = state_space(head_values, write_values, read_values, step_length_value, decay_rate_logs)
    gated = scan_out * jax.nn.silu(output_gate_inputs.astype(jnp.float32))
    grouped = gated.reshape(length, GROUPS, HEADS * HEAD_DIM // GROUPS)
    grouped = grouped * lax.rsqrt(lax.optimization_barrier(jnp.mean(grouped * grouped, axis=-1, keepdims=True)) + eps_norm)
    mixer_normed = (grouped.reshape(length, HEADS * HEAD_DIM) * grouped_norm_gain).astype(jnp.bfloat16)
    mixer_result = jnp.dot(mixer_normed, mixer_output_weight, preferred_element_type=jnp.float32).astype(jnp.bfloat16)
    rows_float = expert_input_rows.astype(jnp.float32)
    moe_normed = (rows_float * lax.rsqrt(lax.optimization_barrier(jnp.mean(rows_float * rows_float, axis=-1, keepdims=True)) + eps_norm) * expert_norm_gain).astype(jnp.bfloat16)
    score_float = router_chosen_scores.astype(jnp.float32)
    route_weight = score_float / lax.optimization_barrier(jnp.sum(score_float, axis=-1, keepdims=True)) * route_scale
    token_total = expert_input_rows.shape[0]
    device_total = token_total // MOE_ROWS
    flat_expert = routes.reshape(device_total, MOE_ROWS * TOP_K)
    onehot = (flat_expert[:, :, None] == jnp.arange(EXPERTS, dtype=jnp.int32)[None, None, :]).astype(jnp.int32)
    before = jnp.cumsum(onehot, axis=1) - onehot
    slot_rank = lax.optimization_barrier(jnp.sum(before * onehot, axis=2))
    slot_index = jnp.arange(device_total, dtype=jnp.int32)[:, None] * CAPACITY + slot_rank
    token_index = jnp.arange(token_total * TOP_K, dtype=jnp.int32) // TOP_K
    table_token = jnp.full((EXPERTS, device_total * CAPACITY), token_total, jnp.int32).at[flat_expert.reshape(-1), slot_index.reshape(-1)].set(token_index)
    table_weight = jnp.zeros((EXPERTS, device_total * CAPACITY), jnp.float32).at[flat_expert.reshape(-1), slot_index.reshape(-1)].set(route_weight.reshape(-1))
    padded_rows = jnp.concatenate([moe_normed, jnp.zeros((1, D), jnp.bfloat16)], axis=0)
    slice_width = EXPERT_FF // N_TP

    def one_expert(running_sum, expert_data):
        tokens_here, weights_here, gate_weight, up_weight, down_weight = expert_data
        picked = padded_rows[tokens_here]
        gate_value = jnp.dot(picked, gate_weight, preferred_element_type=jnp.float32)
        up_value = jnp.dot(picked, up_weight, preferred_element_type=jnp.float32)
        hidden = (jax.nn.silu(gate_value) * up_value).astype(jnp.bfloat16)
        summed = jnp.zeros((picked.shape[0], D), jnp.float32)
        for slice_index in range(N_TP):
            lower_edge = slice_index * slice_width
            part = jnp.dot(hidden[:, lower_edge:lower_edge + slice_width], down_weight[lower_edge:lower_edge + slice_width], preferred_element_type=jnp.float32).astype(jnp.bfloat16)
            summed = summed + part.astype(jnp.float32)
        return (running_sum.at[tokens_here].add(summed * weights_here[:, None]), None)
    routed, _ = lax.scan(one_expert, jnp.zeros((token_total + 1, D), jnp.float32), (table_token, table_weight, routed_gate_weight, routed_up_weight, routed_down_weight))
    shared_hidden = (jax.nn.silu(jnp.dot(moe_normed, shared_gate_weight, preferred_element_type=jnp.float32)) * jnp.dot(moe_normed, shared_up_weight, preferred_element_type=jnp.float32)).astype(jnp.bfloat16)
    shared_total = jnp.dot(shared_hidden, shared_down_weight, preferred_element_type=jnp.float32)
    moe_result = (shared_total + routed[:token_total]).astype(jnp.bfloat16)
    return (mixer_result, moe_result)
```

```python
import jax
import jax.numpy as jnp
from jax import lax
from jax.sharding import PartitionSpec as P

HEAD_DIM = 64
STATE = 128
BLOCK = 64


eps_norm = 1e-06
route_scale = 2.5
highest = lax.Precision.HIGHEST


def from_behind(value, axis, by):
    devices = lax.axis_size(axis)
    pairs = [(i, i + by) for i in range(devices) if 0 <= i + by < devices]
    return lax.ppermute(value, axis, pairs)


def carried_in(decay, state, axis):
    count, mine = (lax.axis_size(axis), lax.axis_index(axis))
    heads = decay.size
    width = state.shape[-1]
    flat_decay = decay.reshape(heads)
    parts, rest = [], flat_decay
    for _ in range(3):
        part = lax.reduce_precision(rest, exponent_bits=8, mantissa_bits=7)
        parts.append(part)
        rest = rest - part
    decay_rows = jnp.pad(jnp.stack(parts, axis=1), ((0, 0), (0, width - 3)))
    packed = jnp.concatenate([state.reshape(-1, width), decay_rows], axis=0).astype(jnp.bfloat16)
    pieces = lax.all_gather(packed, axis).astype(jnp.float32)
    decays = jnp.sum(pieces[:, -heads:, :3], axis=-1)
    order = jnp.arange(count, dtype=jnp.int32)
    between = (order[None, :] > order[:, None]) & (order[None, :] < mine)
    spans = jnp.sum(jnp.where(between[:, :, None], decays[None], 0.0), axis=1)
    ratio = jnp.where((order < mine)[:, None], jnp.exp(spans), 0.0)
    states = pieces[:, :-heads].reshape((count, heads) + state.shape[-2:])
    return jnp.sum(states * ratio[:, :, None, None], axis=0).reshape(state.shape)


def conv_silu(values, weights):
    taps = weights.shape[0]
    length = values.shape[0] - taps + 1
    running_sum = jnp.zeros((length, values.shape[1]), jnp.float32)
    for offset in range(taps):
        running_sum = running_sum + weights[offset].astype(jnp.float32) * values[
            offset : offset + length
        ].astype(jnp.float32)
    return jax.nn.silu(running_sum)


def tail_rows_from_behind(head_inputs, write_vectors, read_vectors, taps):
    start = head_inputs.shape[0] - taps + 1
    tail_rows = jnp.concatenate([head_inputs[start:], write_vectors[start:], read_vectors[start:]], axis=1)
    return from_behind(tail_rows, "ep", 1)


def mixer_rows(
    earlier,
    head_inputs_unfiltered,
    group_write_vectors,
    group_read_vectors,
    output_gate_inputs,
    step_preactivation,
    extra_decay_logs,
    head_decay_logs,
    head_filter_taps,
    write_filter_taps,
    read_filter_taps,
    grouped_norm_gain,
):
    row_total = head_inputs_unfiltered.shape[0]
    head_chans = head_inputs_unfiltered.shape[1]
    write_chans = group_write_vectors.shape[1]
    padded_heads = jnp.concatenate([earlier[:, :head_chans], head_inputs_unfiltered], axis=0)
    padded_write = jnp.concatenate(
        [earlier[:, head_chans : head_chans + write_chans], group_write_vectors], axis=0
    )
    padded_read = jnp.concatenate(
        [earlier[:, head_chans + write_chans :], group_read_vectors], axis=0
    )
    heads_local = step_preactivation.shape[0]
    groups_local = write_chans // STATE
    per_group = heads_local // groups_local
    block_count = row_total // BLOCK
    head_values = conv_silu(padded_heads, head_filter_taps).reshape(
        block_count, BLOCK, groups_local, per_group, HEAD_DIM
    )
    write_values = conv_silu(padded_write, write_filter_taps).reshape(
        block_count, BLOCK, groups_local, STATE
    )
    read_values = conv_silu(padded_read, read_filter_taps).reshape(
        block_count, BLOCK, groups_local, STATE
    )
    step_length_value = jax.nn.softplus(step_preactivation)
    decay_rate_logs = -jnp.exp(head_decay_logs)[:, None] * step_length_value + extra_decay_logs
    step_blocks = step_length_value.reshape(groups_local, per_group, block_count, BLOCK)
    cumulative = jnp.cumsum(
        decay_rate_logs.reshape(groups_local, per_group, block_count, BLOCK), axis=3
    )
    weighted = head_values * jnp.transpose(step_blocks, (2, 3, 0, 1))[..., None]
    lower_mask = jnp.tril(jnp.ones((BLOCK, BLOCK), bool))
    gap_logs = cumulative[..., :, None] - cumulative[..., None, :]
    within = jnp.exp(jnp.where(lower_mask, gap_logs, -jnp.inf))
    affinity = jnp.einsum("blgn,bsgn->gbls", read_values, write_values, precision=highest)
    local_part = jnp.einsum(
        "gebls,bsgep->blgep", affinity[:, None] * within, weighted, precision=highest
    )
    to_end = jnp.exp(cumulative[..., -1:] - cumulative)
    block_states = jnp.einsum(
        "bsgn,bsgep,gebs->bgepn", write_values, weighted, to_end, precision=highest
    )
    block_decay = cumulative[..., -1]
    running = jnp.cumsum(block_decay, axis=2)
    entering = running - block_decay
    earlier_blocks = jnp.tril(jnp.ones((block_count, block_count), bool), -1)
    block_ratio = entering[..., :, None] - running[..., None, :]
    carry_weights = jnp.exp(jnp.where(earlier_blocks, block_ratio, -jnp.inf))
    inside = jnp.einsum("gebc,cgepn->bgepn", carry_weights, block_states, precision=highest)
    device_decay = running[..., -1]
    device_state = jnp.einsum(
        "gec,cgepn->gepn",
        jnp.exp(device_decay[..., None] - running),
        block_states,
        precision=highest,
    )
    incoming = carried_in(device_decay, device_state, "ep")
    states_in = (
        inside + jnp.exp(jnp.transpose(entering, (2, 0, 1)))[..., None, None] * incoming[None]
    )
    carried_part = (
        jnp.einsum("blgn,bgepn->blgep", read_values, states_in, precision=highest)
        * jnp.transpose(jnp.exp(cumulative), (2, 3, 0, 1))[..., None]
    )
    scan_out = (local_part + carried_part).reshape(row_total, groups_local, per_group * HEAD_DIM)
    gate_values = jax.nn.silu(output_gate_inputs.astype(jnp.float32)).reshape(
        row_total, groups_local, per_group * HEAD_DIM
    )
    gated_rows = scan_out * gate_values
    gated_rows = gated_rows * lax.rsqrt(
        jnp.mean(gated_rows * gated_rows, axis=-1, keepdims=True) + eps_norm
    )
    return (gated_rows.reshape(row_total, head_chans) * grouped_norm_gain).astype(jnp.bfloat16)


def local(
    head_inputs_unfiltered,
    group_write_vectors,
    group_read_vectors,
    output_gate_inputs,
    step_preactivation,
    extra_decay_logs,
    head_decay_logs,
    head_filter_taps,
    write_filter_taps,
    read_filter_taps,
    grouped_norm_gain,
    mixer_output_weight,
    expert_input_rows,
    expert_norm_gain,
    routes,
    router_chosen_scores,
    routed_gate_weight,
    routed_up_weight,
    routed_down_weight,
    shared_gate_weight,
    shared_up_weight,
    shared_down_weight,
):
    earlier = tail_rows_from_behind(
        head_inputs_unfiltered, group_write_vectors, group_read_vectors, head_filter_taps.shape[0]
    )
    tp_count = lax.axis_size("tp")
    ep_count = lax.axis_size("ep")
    tok_local = expert_input_rows.shape[0]
    model_width = expert_input_rows.shape[1]
    top_count = routes.shape[1]
    local_experts = routed_gate_weight.shape[0]
    experts = local_experts * ep_count
    capacity = 3 * tok_local * top_count // (2 * experts)
    rows_float = expert_input_rows.astype(jnp.float32)
    normed = (
        rows_float
        * lax.rsqrt(jnp.mean(rows_float * rows_float, axis=-1, keepdims=True) + eps_norm)
        * expert_norm_gain
    ).astype(jnp.bfloat16)
    score_float = router_chosen_scores.astype(jnp.float32)
    weights = score_float / jnp.sum(score_float, axis=1, keepdims=True) * route_scale
    choice = routes[None, :, :] == jnp.arange(experts, dtype=jnp.int32)[:, None, None]
    named = jnp.any(choice, axis=2)
    weight_of = jnp.sum(jnp.where(choice, weights[None], 0.0), axis=2)
    row_order = jnp.arange(tok_local, dtype=jnp.int32)
    earlier_rows = (row_order[:, None] < row_order[None, :]).astype(jnp.bfloat16)
    rank = jnp.dot(
        named.astype(jnp.bfloat16), earlier_rows, preferred_element_type=jnp.float32
    ).astype(jnp.int32)

    cuts = [0, capacity // 2, capacity] if capacity > 1 else [0, capacity]
    picks, outgoing = [], []
    for low, high in zip(cuts[:-1], cuts[1:]):
        places = jnp.arange(low, high, dtype=jnp.int32)
        picked = named[:, None, :] & (rank[:, None, :] == places[None, :, None])
        picks.append(picked)
        outgoing.append(
            jnp.dot(
                picked.reshape(-1, tok_local).astype(jnp.bfloat16),
                normed,
                preferred_element_type=jnp.float32,
            ).astype(jnp.bfloat16)
        )
    earlier, outgoing[0] = lax.optimization_barrier((earlier, outgoing[0]))
    group_rows = lax.all_gather(normed, "tp", axis=0, tiled=True)

    arrived = []
    for block in outgoing:
        arrived.append(lax.all_to_all(block, "ep", split_axis=0, concat_axis=0, tiled=True))
    gathered = [lax.all_gather(block, "tp", axis=0) for block in arrived]

    shared_hidden = (
        jax.nn.silu(jnp.dot(group_rows, shared_gate_weight, preferred_element_type=jnp.float32))
        * jnp.dot(group_rows, shared_up_weight, preferred_element_type=jnp.float32)
    ).astype(jnp.bfloat16)
    shared_part = jnp.dot(shared_hidden, shared_down_weight, preferred_element_type=jnp.float32)

    mixer_normed = mixer_rows(
        earlier,
        head_inputs_unfiltered,
        group_write_vectors,
        group_read_vectors,
        output_gate_inputs,
        step_preactivation,
        extra_decay_logs,
        head_decay_logs,
        head_filter_taps,
        write_filter_taps,
        read_filter_taps,
        grouped_norm_gain,
    )

    def expert_rows(block):
        sources = block.reshape(tp_count, ep_count, local_experts, -1, model_width)
        gate_value = jnp.einsum(
            "osecd,edf->osecf", sources, routed_gate_weight, preferred_element_type=jnp.float32
        )
        up_value = jnp.einsum(
            "osecd,edf->osecf", sources, routed_up_weight, preferred_element_type=jnp.float32
        )
        hidden = (jax.nn.silu(gate_value) * up_value).astype(jnp.bfloat16)
        partial_value = jnp.einsum(
            "osecf,efd->osecd", hidden, routed_down_weight, preferred_element_type=jnp.float32
        ).astype(jnp.bfloat16)
        return lax.psum_scatter(
            partial_value.reshape(-1, model_width), "tp", scatter_dimension=0, tiled=True
        )

    own_term = jnp.zeros((tok_local, model_width), jnp.float32)
    for block, picked in zip(gathered, picks):
        returned = lax.all_to_all(
            expert_rows(block), "ep", split_axis=0, concat_axis=0, tiled=True
        )
        mixing = jnp.where(picked, weight_of[:, None, :], 0.0).reshape(-1, tok_local)
        own_term = own_term + jnp.einsum(
            "sr,sd->rd", mixing, returned.astype(jnp.float32), precision=highest
        )
    mix_block = mixer_normed.shape[0] // tp_count
    block_rows = mix_block + tok_local
    mix_term = jnp.dot(
        mixer_normed, mixer_output_weight, preferred_element_type=jnp.float32
    ).astype(jnp.bfloat16).reshape(tp_count, mix_block, model_width)
    moe_term = shared_part.astype(jnp.bfloat16).reshape(tp_count, tok_local, model_width)
    row_sums = lax.psum_scatter(
        jnp.concatenate([mix_term, moe_term], axis=1).reshape(tp_count * block_rows, model_width),
        "tp",
        scatter_dimension=0,
        tiled=True,
    )
    mixer_result = row_sums[:mix_block]
    moe_total = row_sums[mix_block:].astype(jnp.float32) + own_term
    return (mixer_result.astype(jnp.bfloat16), moe_total.astype(jnp.bfloat16))


def solution(mesh):
    in_specs = (
        P("ep", "tp"),
        P("ep", "tp"),
        P("ep", "tp"),
        P("ep", "tp"),
        P("tp", "ep"),
        P("tp", "ep"),
        P("tp"),
        P(None, "tp"),
        P(None, "tp"),
        P(None, "tp"),
        P("tp"),
        P("tp", None),
        P(("ep", "tp"), None),
        P(),
        P(("ep", "tp"), None),
        P(("ep", "tp"), None),
        P("ep", None, "tp"),
        P("ep", None, "tp"),
        P("ep", "tp", None),
        P(None, "tp"),
        P(None, "tp"),
        P("tp", None),
    )
    out_specs = (P(("ep", "tp"), None), P(("ep", "tp"), None))
    return jax.shard_map(local, mesh=mesh, in_specs=in_specs, out_specs=out_specs, check_vma=False)
```

```python
import jax
import jax.numpy as jnp
from jax import lax
from jax.sharding import PartitionSpec as P

HEAD_DIM = 64
STATE = 128
BLOCK = 64


eps_norm = 1e-06
route_scale = 2.5
highest = lax.Precision.HIGHEST


def from_behind(value, axis, by):
    devices = lax.axis_size(axis)
    pairs = [(i, i + by) for i in range(devices) if 0 <= i + by < devices]
    return lax.ppermute(value, axis, pairs)


def sent_state(decay, state, axis, by):
    heads, width = decay.shape[0], state.shape[-1]
    parts, rest = [], decay
    for _ in range(3):
        part = lax.reduce_precision(rest, exponent_bits=8, mantissa_bits=7)
        parts.append(part)
        rest = rest - part
    decay_rows = jnp.pad(jnp.stack(parts, axis=1), ((0, 0), (0, width - 3)))
    packed = jnp.concatenate([state.reshape(-1, width), decay_rows], axis=0).astype(jnp.bfloat16)
    packed = from_behind(packed, axis, by).astype(jnp.float32)
    return jnp.sum(packed[-heads:, :3], axis=-1), packed[:-heads].reshape(state.shape)


def carried_in(decay, state, axis):
    shape = state.shape
    own = (decay.reshape(-1), state.reshape((-1,) + shape[-2:]))
    before, by = None, 1
    while by < lax.axis_size(axis):
        span = own if before is None else combine_states(before, own)
        received = sent_state(*span, axis, by)
        before = received if before is None else combine_states(received, before)
        by *= 2
    if before is None:
        return jnp.zeros_like(state)
    return before[1].reshape(shape)


def combine_states(earlier_part, later_part):
    return (
        earlier_part[0] + later_part[0],
        later_part[1] + jnp.exp(later_part[0])[..., None, None] * earlier_part[1],
    )


def conv_silu(values, weights):
    taps = weights.shape[0]
    length = values.shape[0] - taps + 1
    running_sum = jnp.zeros((length, values.shape[1]), jnp.float32)
    for offset in range(taps):
        running_sum = running_sum + weights[offset].astype(jnp.float32) * values[
            offset : offset + length
        ].astype(jnp.float32)
    return jax.nn.silu(running_sum)


def tail_rows_from_behind(head_inputs, write_vectors, read_vectors, taps):
    start = head_inputs.shape[0] - taps + 1
    tail_rows = jnp.concatenate([head_inputs[start:], write_vectors[start:], read_vectors[start:]], axis=1)
    return from_behind(tail_rows, "ep", 1)


def mixer_rows(
    earlier,
    head_inputs_unfiltered,
    group_write_vectors,
    group_read_vectors,
    output_gate_inputs,
    step_preactivation,
    extra_decay_logs,
    head_decay_logs,
    head_filter_taps,
    write_filter_taps,
    read_filter_taps,
    grouped_norm_gain,
):
    row_total = head_inputs_unfiltered.shape[0]
    head_chans = head_inputs_unfiltered.shape[1]
    write_chans = group_write_vectors.shape[1]
    padded_heads = jnp.concatenate([earlier[:, :head_chans], head_inputs_unfiltered], axis=0)
    padded_write = jnp.concatenate(
        [earlier[:, head_chans : head_chans + write_chans], group_write_vectors], axis=0
    )
    padded_read = jnp.concatenate(
        [earlier[:, head_chans + write_chans :], group_read_vectors], axis=0
    )
    heads_local = step_preactivation.shape[0]
    groups_local = write_chans // STATE
    per_group = heads_local // groups_local
    block_count = row_total // BLOCK
    head_values = conv_silu(padded_heads, head_filter_taps).reshape(
        block_count, BLOCK, groups_local, per_group, HEAD_DIM
    )
    write_values = conv_silu(padded_write, write_filter_taps).reshape(
        block_count, BLOCK, groups_local, STATE
    )
    read_values = conv_silu(padded_read, read_filter_taps).reshape(
        block_count, BLOCK, groups_local, STATE
    )
    step_length_value = jax.nn.softplus(step_preactivation)
    decay_rate_logs = -jnp.exp(head_decay_logs)[:, None] * step_length_value + extra_decay_logs
    step_blocks = step_length_value.reshape(groups_local, per_group, block_count, BLOCK)
    cumulative = jnp.cumsum(
        decay_rate_logs.reshape(groups_local, per_group, block_count, BLOCK), axis=3
    )
    weighted = head_values * jnp.transpose(step_blocks, (2, 3, 0, 1))[..., None]
    lower_mask = jnp.tril(jnp.ones((BLOCK, BLOCK), bool))
    gap_logs = cumulative[..., :, None] - cumulative[..., None, :]
    within = jnp.exp(jnp.where(lower_mask, gap_logs, -jnp.inf))
    affinity = jnp.einsum("blgn,bsgn->gbls", read_values, write_values, precision=highest)
    local_part = jnp.einsum(
        "gebls,bsgep->blgep", affinity[:, None] * within, weighted, precision=highest
    )
    to_end = jnp.exp(cumulative[..., -1:] - cumulative)
    block_states = jnp.einsum(
        "bsgn,bsgep,gebs->bgepn", write_values, weighted, to_end, precision=highest
    )
    block_decay = cumulative[..., -1]
    running = jnp.cumsum(block_decay, axis=2)
    entering = running - block_decay
    earlier_blocks = jnp.tril(jnp.ones((block_count, block_count), bool), -1)
    block_ratio = entering[..., :, None] - running[..., None, :]
    carry_weights = jnp.exp(jnp.where(earlier_blocks, block_ratio, -jnp.inf))
    inside = jnp.einsum("gebc,cgepn->bgepn", carry_weights, block_states, precision=highest)
    device_decay = running[..., -1]
    device_state = jnp.einsum(
        "gec,cgepn->gepn",
        jnp.exp(device_decay[..., None] - running),
        block_states,
        precision=highest,
    )
    incoming = carried_in(device_decay, device_state, "ep")
    states_in = (
        inside + jnp.exp(jnp.transpose(entering, (2, 0, 1)))[..., None, None] * incoming[None]
    )
    carried_part = (
        jnp.einsum("blgn,bgepn->blgep", read_values, states_in, precision=highest)
        * jnp.transpose(jnp.exp(cumulative), (2, 3, 0, 1))[..., None]
    )
    scan_out = (local_part + carried_part).reshape(row_total, groups_local, per_group * HEAD_DIM)
    gate_values = jax.nn.silu(output_gate_inputs.astype(jnp.float32)).reshape(
        row_total, groups_local, per_group * HEAD_DIM
    )
    gated_rows = scan_out * gate_values
    gated_rows = gated_rows * lax.rsqrt(
        jnp.mean(gated_rows * gated_rows, axis=-1, keepdims=True) + eps_norm
    )
    return (gated_rows.reshape(row_total, head_chans) * grouped_norm_gain).astype(jnp.bfloat16)


def local(
    head_inputs_unfiltered,
    group_write_vectors,
    group_read_vectors,
    output_gate_inputs,
    step_preactivation,
    extra_decay_logs,
    head_decay_logs,
    head_filter_taps,
    write_filter_taps,
    read_filter_taps,
    grouped_norm_gain,
    mixer_output_weight,
    expert_input_rows,
    expert_norm_gain,
    routes,
    router_chosen_scores,
    routed_gate_weight,
    routed_up_weight,
    routed_down_weight,
    shared_gate_weight,
    shared_up_weight,
    shared_down_weight,
):
    earlier = tail_rows_from_behind(
        head_inputs_unfiltered, group_write_vectors, group_read_vectors, head_filter_taps.shape[0]
    )
    tp_count = lax.axis_size("tp")
    ep_count = lax.axis_size("ep")
    tok_local = expert_input_rows.shape[0]
    model_width = expert_input_rows.shape[1]
    top_count = routes.shape[1]
    local_experts = routed_gate_weight.shape[0]
    experts = local_experts * ep_count
    capacity = 3 * tok_local * top_count // (2 * experts)
    rows_float = expert_input_rows.astype(jnp.float32)
    normed = (
        rows_float
        * lax.rsqrt(jnp.mean(rows_float * rows_float, axis=-1, keepdims=True) + eps_norm)
        * expert_norm_gain
    ).astype(jnp.bfloat16)
    score_float = router_chosen_scores.astype(jnp.float32)
    weights = score_float / jnp.sum(score_float, axis=1, keepdims=True) * route_scale
    choice = routes[None, :, :] == jnp.arange(experts, dtype=jnp.int32)[:, None, None]
    named = jnp.any(choice, axis=2)
    weight_of = jnp.sum(jnp.where(choice, weights[None], 0.0), axis=2)
    row_order = jnp.arange(tok_local, dtype=jnp.int32)
    earlier_rows = (row_order[:, None] < row_order[None, :]).astype(jnp.bfloat16)
    rank = jnp.dot(
        named.astype(jnp.bfloat16), earlier_rows, preferred_element_type=jnp.float32
    ).astype(jnp.int32)

    cuts = [0, capacity // 2, capacity] if capacity > 1 else [0, capacity]
    picks, outgoing = [], []
    for low, high in zip(cuts[:-1], cuts[1:]):
        places = jnp.arange(low, high, dtype=jnp.int32)
        picked = named[:, None, :] & (rank[:, None, :] == places[None, :, None])
        picks.append(picked)
        outgoing.append(
            jnp.dot(
                picked.reshape(-1, tok_local).astype(jnp.bfloat16),
                normed,
                preferred_element_type=jnp.float32,
            ).astype(jnp.bfloat16)
        )
    group_rows = lax.all_gather(normed, "tp", axis=0, tiled=True)
    earlier, group_rows, outgoing[0] = lax.optimization_barrier((earlier, group_rows, outgoing[0]))

    arrived = []
    for block in outgoing:
        arrived.append(lax.all_to_all(block, "ep", split_axis=0, concat_axis=0, tiled=True))
    gathered = [lax.all_gather(block, "tp", axis=0) for block in arrived]

    shared_hidden = (
        jax.nn.silu(jnp.dot(group_rows, shared_gate_weight, preferred_element_type=jnp.float32))
        * jnp.dot(group_rows, shared_up_weight, preferred_element_type=jnp.float32)
    ).astype(jnp.bfloat16)
    shared_part = jnp.dot(shared_hidden, shared_down_weight, preferred_element_type=jnp.float32)

    mixer_normed = mixer_rows(
        earlier,
        head_inputs_unfiltered,
        group_write_vectors,
        group_read_vectors,
        output_gate_inputs,
        step_preactivation,
        extra_decay_logs,
        head_decay_logs,
        head_filter_taps,
        write_filter_taps,
        read_filter_taps,
        grouped_norm_gain,
    )

    def expert_rows(block):
        sources = block.reshape(tp_count, ep_count, local_experts, -1, model_width)
        gate_value = jnp.einsum(
            "osecd,edf->osecf", sources, routed_gate_weight, preferred_element_type=jnp.float32
        )
        up_value = jnp.einsum(
            "osecd,edf->osecf", sources, routed_up_weight, preferred_element_type=jnp.float32
        )
        hidden = (jax.nn.silu(gate_value) * up_value).astype(jnp.bfloat16)
        partial_value = jnp.einsum(
            "osecf,efd->osecd", hidden, routed_down_weight, preferred_element_type=jnp.float32
        ).astype(jnp.bfloat16)
        return lax.psum_scatter(
            partial_value.reshape(-1, model_width), "tp", scatter_dimension=0, tiled=True
        )

    own_term = jnp.zeros((tok_local, model_width), jnp.float32)
    for block, picked in zip(gathered, picks):
        returned = lax.all_to_all(
            expert_rows(block), "ep", split_axis=0, concat_axis=0, tiled=True
        )
        mixing = jnp.where(picked, weight_of[:, None, :], 0.0).reshape(-1, tok_local)
        own_term = own_term + jnp.einsum(
            "sr,sd->rd", mixing, returned.astype(jnp.float32), precision=highest
        )
    mix_block = mixer_normed.shape[0] // tp_count
    block_rows = mix_block + tok_local
    mix_term = jnp.dot(
        mixer_normed, mixer_output_weight, preferred_element_type=jnp.float32
    ).astype(jnp.bfloat16).reshape(tp_count, mix_block, model_width)
    moe_term = shared_part.astype(jnp.bfloat16).reshape(tp_count, tok_local, model_width)
    row_sums = lax.psum_scatter(
        jnp.concatenate([mix_term, moe_term], axis=1).reshape(tp_count * block_rows, model_width),
        "tp",
        scatter_dimension=0,
        tiled=True,
    )
    mixer_result = row_sums[:mix_block]
    moe_total = row_sums[mix_block:].astype(jnp.float32) + own_term
    return (mixer_result.astype(jnp.bfloat16), moe_total.astype(jnp.bfloat16))


def solution(mesh):
    in_specs = (
        P("ep", "tp"),
        P("ep", "tp"),
        P("ep", "tp"),
        P("ep", "tp"),
        P("tp", "ep"),
        P("tp", "ep"),
        P("tp"),
        P(None, "tp"),
        P(None, "tp"),
        P(None, "tp"),
        P("tp"),
        P("tp", None),
        P(("ep", "tp"), None),
        P(),
        P(("ep", "tp"), None),
        P(("ep", "tp"), None),
        P("ep", None, "tp"),
        P("ep", None, "tp"),
        P("ep", "tp", None),
        P(None, "tp"),
        P(None, "tp"),
        P("tp", None),
    )
    out_specs = (P(("ep", "tp"), None), P(("ep", "tp"), None))
    return jax.shard_map(local, mesh=mesh, in_specs=in_specs, out_specs=out_specs, check_vma=False)
```
